32 devices in a mesh: tp: 4 (over y, x), dp: 8 (over z, core).
Axes of the slice: x: 2, y: 2, z: 4, core: 2. Of those that a mesh axis runs over, the one named last changes fastest.
Arguments:
- tokens: bfloat16 [16, 4096], P('tp', 'dp'), may hold values from -12.5 to 12.5
- gain_first: bfloat16 [4096], P('dp'), may hold values from 0.099609375 to 1.8984375
- query_first: bfloat16 [4096, 2048], P('dp', 'tp'), may hold values from -0.09375 to 0.09375
- key_first: bfloat16 [4096, 2048], P('dp', 'tp'), may hold values from -0.09375 to 0.09375
- value_first: bfloat16 [4096, 4096], P('dp', 'tp'), may hold values from -0.09375 to 0.09375
- outgate_first: bfloat16 [4096, 4096], P('dp', 'tp'), may hold values from -0.09375 to 0.09375
- inputgate_first: bfloat16 [4096, 16], P('dp'), may hold values from -0.09375 to 0.09375
- forget_first: bfloat16 [4096, 16], P('dp'), may hold values from -0.09375 to 0.09375
- mixing_first: bfloat16 [4096, 4096], P('tp', 'dp'), may hold values from -0.09375 to 0.09375
- cell_first: float32 [16, 16, 256, 128], P('dp', 'tp'), may hold values from -6 to 6
- norm_first: float32 [16, 16, 128], P('dp', 'tp'), may hold values from -6 to 6
- stabilizer_first: float32 [16, 16], P('dp', 'tp'), may hold values from -3 to 115
- gain_second: bfloat16 [4096], P('dp'), may hold values from 0.099609375 to 1.8984375
- query_second: bfloat16 [4096, 2048], P('dp', 'tp'), may hold values from -0.09375 to 0.09375
- key_second: bfloat16 [4096, 2048], P('dp', 'tp'), may hold values from -0.09375 to 0.09375
- value_second: bfloat16 [4096, 4096], P('dp', 'tp'), may hold values from -0.09375 to 0.09375
- outgate_second: bfloat16 [4096, 4096], P('dp', 'tp'), may hold values from -0.09375 to 0.09375
- inputgate_second: bfloat16 [4096, 16], P('dp'), may hold values from -0.09375 to 0.09375
- forget_second: bfloat16 [4096, 16], P('dp'), may hold values from -0.09375 to 0.09375
- mixing_second: bfloat16 [4096, 4096], P('tp', 'dp'), may hold values from -0.09375 to 0.09375
- cell_second: float32 [16, 16, 256, 128], P('dp', 'tp'), may hold values from -6 to 6
- norm_second: float32 [16, 16, 128], P('dp', 'tp'), may hold values from -6 to 6
- stabilizer_second: float32 [16, 16], P('dp', 'tp'), may hold values from -3 to 115
Outputs:
- hidden: bfloat16 [16, 4096], P('tp', 'dp')
- cell_first_next: float32 [16, 16, 256, 128], P('dp', 'tp')
- norm_first_next: float32 [16, 16, 128], P('dp', 'tp')
- stabilizer_first_next: float32 [16, 16], P('dp', 'tp')
- cell_second_next: float32 [16, 16, 256, 128], P('dp', 'tp')
- norm_second_next: float32 [16, 16, 128], P('dp', 'tp')
- stabilizer_second_next: float32 [16, 16], P('dp', 'tp')
The draws below stay inside these ranges and needn't reach their ends.
All inputs are finite; a program needn't handle non-finite values.
Results may differ from the reference program's by a relative error of at most 0.023.
Values may be sent and summed in bfloat16 or wider, within the bound.
No kernel may reach another device: no remote copies, remote signals or barrier semaphores. Data moves between devices by JAX's collectives and lax.ppermute only.
A program may use at most 64 MiB of HBM per device.

```python
import jax
import jax.numpy as jnp
from jax import lax

D = 4096
HEADS = 16
DHK = 128
DHV = 256
BATCH = 16


def stabilizer_law(key):
    first_key = jax.random.fold_in(key, 0)
    base = jax.random.uniform(first_key, (BATCH, HEADS), jnp.float32, -3.0, 3.0)
    return base


def draw_stabilizer_first(key, part):
    return stabilizer_law(jax.random.fold_in(key, 1))


def draw_stabilizer_second(key, part):
    return stabilizer_law(jax.random.fold_in(key, 2))


def draw_tokens(key, part):
    own_key = jax.random.fold_in(key, 5)
    first_key = jax.random.fold_in(own_key, 0)
    noise = jnp.clip(jax.random.normal(first_key, (BATCH, D), jnp.float32), -4.0, 4.0)
    ramp = jnp.exp(jnp.linspace(-0.7, 0.7, D, dtype=jnp.float32))
    return (noise * ramp[None, :]).astype(jnp.bfloat16)


def block_scale(rng, shape, cuts, low, top_value):
    level = 1.0
    for dim, blocks in cuts:
        heights = jax.random.uniform(jax.random.fold_in(jax.random.fold_in(rng, 6), dim), (blocks,), jnp.float32, low / len(cuts), top_value / len(cuts))
        level = level * jnp.repeat(jnp.exp(heights), shape[dim] // blocks).reshape((-1,) + (1,) * (len(shape) - 1 - dim))
    return level


def gaussian(key, dims, width, most, shards=(), kind=jnp.bfloat16):
    array = width * jax.random.normal(key, dims, jnp.float32)
    if shards:
        array = array * block_scale(key, dims, shards, -0.22, 0.18)
    return jnp.clip(array, -most, most).astype(kind)


def setup_inputs(seed: int = 0) -> dict:
    splits = jax.random.split(jax.random.key(seed), 24)
    return {
        "tokens": draw_tokens(jax.random.fold_in(splits[23], 71), 0),
        "gain_first": jnp.clip(1.0 + 0.18 * jax.random.normal(splits[1], (D,), jnp.float32), 0.099609375, 1.8984375).astype(jnp.bfloat16),
        "query_first": gaussian(splits[2], (D, HEADS * DHK), D ** -0.5, 0.09375, ((0, 8), (1, 4))),
        "key_first": gaussian(splits[3], (D, HEADS * DHK), D ** -0.5, 0.09375, ((0, 8), (1, 4))),
        "value_first": gaussian(splits[4], (D, HEADS * DHV), D ** -0.5, 0.09375, ((0, 8), (1, 4))),
        "outgate_first": gaussian(splits[5], (D, HEADS * DHV), D ** -0.5, 0.09375, ((0, 8), (1, 4))),
        "inputgate_first": gaussian(splits[6], (D, HEADS), D ** -0.5, 0.09375, ((0, 8),)),
        "forget_first": gaussian(splits[7], (D, HEADS), D ** -0.5, 0.09375, ((0, 8),)),
        "mixing_first": gaussian(splits[8], (HEADS * DHV, D), (HEADS * DHV) ** -0.5, 0.09375, ((0, 4), (1, 8))),
        "cell_first": gaussian(splits[9], (BATCH, HEADS, DHV, DHK), 1.0, 6.0, ((0, 8), (1, 4)), jnp.float32),
        "norm_first": gaussian(splits[10], (BATCH, HEADS, DHK), 1.0, 6.0, ((0, 8), (1, 4)), jnp.float32),
        "stabilizer_first": draw_stabilizer_first(jax.random.fold_in(splits[23], 71), 0),
        "gain_second": jnp.clip(1.0 + 0.18 * jax.random.normal(splits[12], (D,), jnp.float32), 0.099609375, 1.8984375).astype(jnp.bfloat16),
        "query_second": gaussian(splits[13], (D, HEADS * DHK), D ** -0.5, 0.09375, ((0, 8), (1, 4))),
        "key_second": gaussian(splits[14], (D, HEADS * DHK), D ** -0.5, 0.09375, ((0, 8), (1, 4))),
        "value_second": gaussian(splits[15], (D, HEADS * DHV), D ** -0.5, 0.09375, ((0, 8), (1, 4))),
        "outgate_second": gaussian(splits[16], (D, HEADS * DHV), D ** -0.5, 0.09375, ((0, 8), (1, 4))),
        "inputgate_second": gaussian(splits[17], (D, HEADS), D ** -0.5, 0.09375, ((0, 8),)),
        "forget_second": gaussian(splits[18], (D, HEADS), D ** -0.5, 0.09375, ((0, 8),)),
        "mixing_second": gaussian(splits[19], (HEADS * DHV, D), (HEADS * DHV) ** -0.5, 0.09375, ((0, 4), (1, 8))),
        "cell_second": gaussian(splits[20], (BATCH, HEADS, DHV, DHK), 1.0, 6.0, ((0, 8), (1, 4)), jnp.float32),
        "norm_second": gaussian(splits[21], (BATCH, HEADS, DHK), 1.0, 6.0, ((0, 8), (1, 4)), jnp.float32),
        "stabilizer_second": draw_stabilizer_second(jax.random.fold_in(splits[23], 71), 0),
    }


eps = 1e-06

def cell_step(stream, gain, w_query, w_key, w_value, w_outgate, w_input, w_forget, w_mixing, cell_state, norm_state, stabilizer):
    batch_rows = stream.shape[0]
    widened = stream.astype(jnp.float32)
    squares = lax.optimization_barrier(jnp.sum(widened * widened, axis=1))
    row_scale = lax.rsqrt(squares / D + eps)[:, None]
    scaled = (widened * gain.astype(jnp.float32)).astype(jnp.bfloat16)

    def project(weight):
        return jnp.dot(scaled, weight, preferred_element_type=jnp.float32) * row_scale
    queries = project(w_query).reshape(batch_rows, HEADS, DHK) * DHK ** (-0.5)
    key_rows = project(w_key).reshape(batch_rows, HEADS, DHK)
    value_rows = project(w_value).reshape(batch_rows, HEADS, DHV)
    outgate_pre = project(w_outgate)
    input_pre = project(w_input)
    forget_pre = project(w_forget)
    log_forget = jax.nn.log_sigmoid(forget_pre)
    stab_next = jnp.maximum(log_forget + stabilizer, input_pre)
    retain = jnp.exp(log_forget + stabilizer - stab_next)
    admitted = jnp.exp(input_pre - stab_next)
    cell_next = retain[:, :, None, None] * cell_state + admitted[:, :, None, None] * value_rows[:, :, :, None] * key_rows[:, :, None, :]
    norm_next = retain[:, :, None] * norm_state + admitted[:, :, None] * key_rows
    numerator = jnp.einsum('shvd,shd->shv', cell_next, queries, precision=lax.Precision.HIGHEST)
    denominator = jnp.einsum('shd,shd->sh', norm_next, queries, precision=lax.Precision.HIGHEST)
    readout = numerator / jnp.maximum(jnp.abs(denominator), 1.0)[:, :, None]
    gated_rows = (readout.reshape(batch_rows, HEADS * DHV) * jax.nn.sigmoid(outgate_pre)).astype(jnp.bfloat16)
    result = (widened + jnp.dot(gated_rows, w_mixing, preferred_element_type=jnp.float32)).astype(jnp.bfloat16)
    return (result, cell_next, norm_next, stab_next)

def reference(tokens, gain_first, query_first, key_first, value_first, outgate_first, inputgate_first, forget_first, mixing_first, cell_first, norm_first, stabilizer_first, gain_second, query_second, key_second, value_second, outgate_second, inputgate_second, forget_second, mixing_second, cell_second, norm_second, stabilizer_second):
    middle, cell_one, norm_one, stab_one = cell_step(tokens, gain_first, query_first, key_first, value_first, outgate_first, inputgate_first, forget_first, mixing_first, cell_first, norm_first, stabilizer_first)
    hidden, cell_two, norm_two, stab_two = cell_step(middle, gain_second, query_second, key_second, value_second, outgate_second, inputgate_second, forget_second, mixing_second, cell_second, norm_second, stabilizer_second)
    return (hidden, cell_one, norm_one, stab_one, cell_two, norm_two, stab_two)
```

```python
import jax
import jax.numpy as jnp
from jax import lax
from jax.sharding import PartitionSpec as P

eps = 1e-06
LANES = 128
F32 = jnp.float32
BF16 = jnp.bfloat16


def peers(x, axis, size):
    if size <= 4 and size & (size - 1) == 0:
        return [
            lax.ppermute(x, axis, [(i, i ^ k) for i in range(size)])
            for k in range(size - 1, 0, -1)
        ]
    return None


def gather(x, axis, size):
    return lax.all_to_all(
        jnp.broadcast_to(x[None], (size,) + x.shape), axis, 0, 0
    )


def gather_rows(x, axis, size):
    own = peers(x, axis, size)
    if own is None:
        stacked = gather(x, axis, size)
        return stacked.reshape((-1,) + x.shape[1:])
    me = lax.axis_index(axis)
    order = [x] + own[::-1]
    stacked = jnp.zeros((size,) + x.shape, x.dtype)
    for k, piece in enumerate(order):
        stacked = lax.dynamic_update_index_in_dim(stacked, piece, me ^ k, 0)
    return stacked.reshape((-1,) + x.shape[1:])


def sum_over(x, axis, size):
    rounded = x.astype(BF16)
    others = peers(rounded, axis, size)
    if others is None:
        return jnp.sum(gather(rounded, axis, size).astype(F32), axis=0)
    for piece in others:
        x = x + piece.astype(F32)
    return x


def scatter_sum(x, axis, size):
    blocks = x.reshape((size, x.shape[0] // size) + x.shape[1:])
    rounded = blocks.astype(BF16)
    if size <= 4 and size & (size - 1) == 0:
        me = lax.axis_index(axis)
        total = lax.dynamic_index_in_dim(blocks, me, 0, False)
        for k in range(size - 1, 0, -1):
            piece = lax.dynamic_index_in_dim(rounded, me ^ k, 0, False)
            total = total + lax.ppermute(
                piece, axis, [(i, i ^ k) for i in range(size)]
            ).astype(F32)
        return total
    return jnp.sum(lax.all_to_all(rounded, axis, 0, 0).astype(F32), axis=0)


def split(x):
    high = x.astype(BF16)
    return high, (x - high.astype(F32)).astype(BF16)


def cell_step(
    sizes,
    widened,
    gain,
    w_query,
    w_key,
    w_value,
    w_outgate,
    w_input,
    w_forget,
    w_mixing,
    cell_state,
    norm_state,
    stabilizer,
):
    dp = sizes["dp"]
    seq_count, local_heads, dhv, dhk = cell_state.shape
    all_heads = w_input.shape[1]
    width = widened.shape[1] * dp
    squares = jnp.sum(widened * widened, axis=1, keepdims=True)
    scaled = (widened * gain.astype(F32)).astype(BF16)

    def project(weight):
        return jnp.dot(scaled, weight, preferred_element_type=F32)

    small = jnp.concatenate([project(w_input), project(w_forget), squares], axis=1)
    high, low = split(small)
    pad = -(high.shape[1] * 2) % LANES
    payload = jnp.concatenate(
        [project(w).astype(BF16) for w in (w_query, w_key, w_value, w_outgate)]
        + [high, low, jnp.zeros((high.shape[0], pad), BF16)],
        axis=1,
    )
    received = lax.all_to_all(
        payload.reshape(dp, seq_count, payload.shape[1]), "dp", 0, 0
    )
    total = jnp.sum(received.astype(F32), axis=0)
    nk, nv = local_heads * dhk, local_heads * dhv
    base = 2 * (nk + nv)
    wide = 2 * all_heads + 1
    small = total[:, base : base + wide] + total[:, base + wide : base + 2 * wide]
    row_scale = lax.rsqrt(small[:, 2 * all_heads :] / width + eps)
    offset = lax.axis_index("tp") * local_heads
    gates = small * row_scale
    input_pre = lax.dynamic_slice_in_dim(gates, offset, local_heads, 1)
    forget_pre = lax.dynamic_slice_in_dim(gates, offset + all_heads, local_heads, 1)
    queries = (total[:, :nk] * row_scale).reshape(seq_count, local_heads, dhk) * dhk ** (-0.5)
    key_rows = (total[:, nk : 2 * nk] * row_scale).reshape(seq_count, local_heads, dhk)
    value_rows = (total[:, 2 * nk : 2 * nk + nv] * row_scale).reshape(seq_count, local_heads, dhv)
    outgate_pre = total[:, 2 * nk + nv : base] * row_scale
    log_forget = jax.nn.log_sigmoid(forget_pre)
    stab_next = jnp.maximum(log_forget + stabilizer, input_pre)
    retain = jnp.exp(log_forget + stabilizer - stab_next)
    admitted = jnp.exp(input_pre - stab_next)
    cell_next = (
        retain[:, :, None, None] * cell_state
        + admitted[:, :, None, None] * value_rows[:, :, :, None] * key_rows[:, :, None, :]
    )
    norm_next = retain[:, :, None] * norm_state + admitted[:, :, None] * key_rows
    numerator = jnp.einsum("shvd,shd->shv", cell_next, queries, precision=lax.Precision.HIGHEST)
    denominator = jnp.einsum("shd,shd->sh", norm_next, queries, precision=lax.Precision.HIGHEST)
    readout = numerator / jnp.maximum(jnp.abs(denominator), 1.0)[:, :, None]
    gated = (readout.reshape(seq_count, nv) * jax.nn.sigmoid(outgate_pre)).astype(BF16)
    gathered = gather(gated, "dp", dp).reshape(-1, nv)
    partial = jnp.dot(gathered, w_mixing, preferred_element_type=F32)
    return partial, cell_next, norm_next, stab_next


def per_device(sizes, tokens, *args):
    tp = sizes["tp"]
    rows = tokens.shape[0]
    stream = gather_rows(tokens, "tp", tp).astype(F32)
    partial, *first = cell_step(sizes, stream, *args[:11])
    middle = (stream + sum_over(partial, "tp", tp)).astype(BF16)
    partial, *second = cell_step(sizes, middle.astype(F32), *args[11:])
    own = lax.dynamic_slice_in_dim(middle, lax.axis_index("tp") * rows, rows, 0)
    hidden = (own.astype(F32) + scatter_sum(partial, "tp", tp)).astype(BF16)
    return (hidden, *first, *second)


def solution(mesh):
    sizes = dict(mesh.shape)
    weight = P("dp", "tp")
    cell = (
        P("dp"),
        weight,
        weight,
        weight,
        weight,
        P("dp", None),
        P("dp", None),
        P("tp", "dp"),
        P("dp", "tp", None, None),
        P("dp", "tp", None),
        P("dp", "tp"),
    )
    states = cell[-3:]
    return jax.shard_map(
        lambda *args: per_device(sizes, *args),
        mesh=mesh,
        in_specs=(P("tp", "dp"), *cell, *cell),
        out_specs=(P("tp", "dp"), *states, *states),
        check_vma=False,
    )
```

```python
import functools

import jax
import jax.numpy as jnp
from jax import lax
from jax.experimental import pallas as pl
from jax.experimental.pallas import tpu as pltpu
from jax.sharding import PartitionSpec as P

eps = 1e-06
LANES = 128
F32 = jnp.float32
BF16 = jnp.bfloat16
NT = (((1,), (1,)), ((), ()))
TN = (((0,), (0,)), ((), ()))
MIB = 1 << 20


def pairwise(size):
    return size <= 4 and size & (size - 1) == 0


def peers(pieces, axis, size):
    order = sorted(range(1, size), key=lambda k: -bin(k).count("1"))
    got = {}
    for k in order:
        got[k] = lax.ppermute(pieces[k - 1], axis, [(i, i ^ k) for i in range(size)])
    return [got[k] for k in range(1, size)]


def split(x):
    high = x.astype(BF16)
    return high, (x - high.astype(F32)).astype(BF16)


def call(body, outs, scratch, cost, limit, *args):
    return pl.pallas_call(
        body,
        out_shape=outs,
        in_specs=[pl.BlockSpec(memory_space=pltpu.VMEM)] * len(args),
        out_specs=[pl.BlockSpec(memory_space=pltpu.VMEM)] * len(outs),
        scratch_shapes=scratch,
        cost_estimate=pl.CostEstimate(flops=cost, bytes_accessed=cost // 16, transcendentals=0),
        compiler_params=pltpu.CompilerParams(vmem_limit_bytes=limit),
    )(*args)


def pick(blocks, index):
    chosen = blocks[0]
    for j in range(1, len(blocks)):
        chosen = jnp.where(index == j, blocks[j], chosen)
    return chosen


def place(piece_refs, target):
    rows = piece_refs[0].shape[0]
    blocks = [piece[...].astype(F32) for piece in piece_refs]
    me = lax.axis_index("tp")
    for j in range(len(blocks)):
        target[j * rows : (j + 1) * rows, :] = pick(blocks, me ^ j)


def row_blocks(ref, rows):
    return [ref[j * rows : (j + 1) * rows, :] for j in range(ref.shape[0] // rows)]


def project(x, gain_ref, weights, small_ref, payload_ref, y_ref, narrow):
    batch = x.shape[0]
    squares = jnp.sum(x * x, axis=1, keepdims=True)
    scaled = (x * gain_ref[...].astype(F32)).astype(BF16)
    at = 0
    for w_ref in weights:
        width = w_ref.shape[1]
        y_ref[:, at : at + width] = jnp.dot(scaled, w_ref[...], preferred_element_type=F32)
        at += width
    gates = lax.dot_general(scaled, small_ref[...], NT, preferred_element_type=F32)
    lane = lax.broadcasted_iota(jnp.int32, (batch, LANES), 1)
    gates = jnp.where(lane == narrow, squares, gates)
    high = gates.astype(BF16).astype(F32)
    y_ref[:, at : at + LANES] = high
    y_ref[:, at + LANES : at + 2 * LANES] = gates - high
    count, seqs, _ = payload_ref.shape
    for d in range(count):
        payload_ref[d] = y_ref[d * seqs : (d + 1) * seqs, :].astype(BF16)


def first_body(n_pieces, narrow, *refs):
    pieces = refs[:n_pieces]
    gain_ref, wq, wk, wv, wo, small_ref, payload_ref, stream_ref, y_ref = refs[n_pieces:]
    if n_pieces == 1:
        whole = pieces[0][...].astype(F32)
        stream_ref[...] = whole
    else:
        place(pieces, stream_ref)
    project(stream_ref[...], gain_ref, (wq, wk, wv, wo), small_ref, payload_ref, y_ref, narrow)


def second_body(n_pieces, narrow, *refs):
    stream_in, own_ref = refs[:2]
    pieces = refs[2 : 2 + n_pieces]
    gain_ref, wq, wk, wv, wo, small_ref, payload_ref, stream_ref, y_ref = refs[2 + n_pieces :]
    total = own_ref[...]
    for piece in pieces:
        if len(piece.shape) == 3:
            total = total + jnp.sum(piece[...].astype(F32), axis=0)
        else:
            total = total + piece[...].astype(F32)
    x = (stream_in[...] + total).astype(BF16).astype(F32)
    stream_ref[...] = x
    project(x, gain_ref, (wq, wk, wv, wo), small_ref, payload_ref, y_ref, narrow)


def state_body(
    width, received_ref, cell_ref, norm_ref, stab_ref,
    gated_ref, cell_out, norm_out, stab_out, read_ref,
):
    seqs, heads, dhv, dhk = cell_ref.shape
    nk, nv = heads * dhk, heads * dhv
    total = received_ref[0].astype(F32)
    for d in range(1, received_ref.shape[0]):
        total = total + received_ref[d].astype(F32)
    base = 2 * (nk + nv)
    small = total[:, base : base + LANES] + total[:, base + LANES : base + 2 * LANES]
    scale = lax.rsqrt(small[:, 2 * heads : 2 * heads + 1] / width + eps)
    small = small * scale
    input_pre = small[:, :heads]
    forget_pre = small[:, heads : 2 * heads]
    log_forget = jnp.minimum(forget_pre, 0.0) - jnp.log1p(jnp.exp(-jnp.abs(forget_pre)))
    kept = log_forget + stab_ref[...]
    stab_next = jnp.maximum(kept, input_pre)
    stab_out[...] = stab_next
    retain = jnp.exp(kept - stab_next)
    admitted = jnp.exp(input_pre - stab_next)
    queries = total[:, :nk] * (scale * dhk ** (-0.5))
    keys = total[:, nk : 2 * nk] * scale
    values = total[:, 2 * nk : 2 * nk + nv] * scale
    gate = jax.nn.sigmoid(total[:, 2 * nk + nv : base] * scale)
    row = lax.broadcasted_iota(jnp.int32, (8, dhk), 0)
    row_v = lax.broadcasted_iota(jnp.int32, (8, dhv), 0)
    for s in range(seqs):
        for h in range(heads):
            keep = retain[s : s + 1, h : h + 1]
            admit = admitted[s : s + 1, h : h + 1]
            query = queries[s : s + 1, h * dhk : (h + 1) * dhk]
            key = keys[s : s + 1, h * dhk : (h + 1) * dhk]
            value = values[s : s + 1, h * dhv : (h + 1) * dhv] * admit
            norm_next = keep * norm_ref[s, h : h + 1, :] + admit * key
            norm_out[s, h : h + 1, :] = norm_next
            bound = jnp.maximum(jnp.abs(jnp.sum(norm_next * query, axis=1, keepdims=True)), 1.0)
            key_high = key.astype(BF16).astype(F32)
            key_low = key - key_high
            value_high = value.astype(BF16).astype(F32)
            value_low = value - value_high
            left = jnp.where(row_v < 2, value_high, jnp.where(row_v < 4, value_low, 0.0))
            right = jnp.where(row & 1 == 0, key_high, key_low)
            outer = lax.dot_general(
                left.astype(BF16), right.astype(BF16), TN, preferred_element_type=F32
            )
            cell_next = keep * cell_ref[s, h] + outer
            cell_out[s, h] = cell_next
            query_high = query.astype(BF16).astype(F32)
            asks = jnp.where(row == 0, query_high, jnp.where(row == 1, query - query_high, 0.0))
            asks = asks.astype(BF16)
            cell_high = cell_next.astype(BF16)
            read = lax.dot_general(asks, cell_high, NT, preferred_element_type=F32)
            low = (cell_next - cell_high.astype(F32)).astype(BF16)
            read = read + lax.dot_general(asks, low, NT, preferred_element_type=F32)
            numerator = jnp.sum(read, axis=0, keepdims=True)
            read_ref[s : s + 1, h * dhv : (h + 1) * dhv] = numerator / bound
    gated = (read_ref[...] * gate).astype(BF16)
    for d in range(gated_ref.shape[0]):
        gated_ref[d] = gated


def mix(gathered_ref, w_ref, x_ref):
    count, seqs, _ = gathered_ref.shape
    for d in range(count):
        x_ref[d * seqs : (d + 1) * seqs, :] = gathered_ref[d].astype(F32)
    return jnp.dot(x_ref[...].astype(BF16), w_ref[...], preferred_element_type=F32)


def middle_body(gathered_ref, w_ref, sent_ref, own_ref, x_ref):
    partial = mix(gathered_ref, w_ref, x_ref)
    own_ref[...] = partial
    sent_ref[...] = partial.astype(BF16)


def last_body(paired, size, gathered_ref, w_ref, *refs):
    x_ref, y_ref = refs[-2:]
    y_ref[...] = mix(gathered_ref, w_ref, x_ref)
    if not paired:
        sent_ref = refs[0]
        rows = sent_ref.shape[1]
        for k in range(size):
            sent_ref[k] = y_ref[k * rows : (k + 1) * rows, :].astype(BF16)
        return
    rows = refs[0].shape[0]
    blocks = row_blocks(y_ref, rows)
    me = lax.axis_index("tp")
    for k in range(size):
        refs[k][...] = pick(blocks, me ^ k).astype(refs[k].dtype)


def final_body(stream_ref, *refs):
    hidden_ref = refs[-1]
    rows = hidden_ref.shape[0]
    total = pick(row_blocks(stream_ref, rows), lax.axis_index("tp"))
    for piece in refs[:-1]:
        if len(piece.shape) == 3:
            total = total + jnp.sum(piece[...].astype(F32), axis=0)
        else:
            total = total + piece[...].astype(F32)
    hidden_ref[...] = total.astype(BF16)


def own_gates(w_input, w_forget, heads):
    offset = lax.axis_index("tp") * heads
    rows = jnp.concatenate(
        [lax.dynamic_slice_in_dim(w.T, offset, heads, 0) for w in (w_input, w_forget)], axis=0
    )
    return jnp.pad(rows, ((0, LANES - rows.shape[0]), (0, 0)))


def per_device(sizes, tokens, *args):
    tp, dp = sizes["tp"], sizes["dp"]
    paired = pairwise(tp)
    rows, features = tokens.shape
    batch = rows * tp
    cells = (args[:11], args[11:])
    seqs, heads, dhv, dhk = cells[0][8].shape
    nk, nv = heads * dhk, heads * dhv
    payload_width = 2 * (nk + nv) + 2 * LANES
    payload = jax.ShapeDtypeStruct((dp, seqs, payload_width), BF16)
    stream = jax.ShapeDtypeStruct((batch, features), F32)
    gated = jax.ShapeDtypeStruct((dp, seqs, nv), BF16)
    small = [own_gates(cell[5], cell[6], heads) for cell in cells]
    gains = [cell[0].reshape(1, features) for cell in cells]
    project_scratch = [pltpu.VMEM((batch, payload_width), F32)]
    project_cost = 2 * batch * features * payload_width
    mix_scratch = pltpu.VMEM((batch, nv), F32)
    mix_cost = 2 * batch * features * nv
    state_cost = 16 * seqs * nv * dhk

    def exchange_dp(x):
        return lax.all_to_all(x, "dp", 0, 0)

    def update(received, cell):
        return call(
            functools.partial(state_body, features * dp),
            [
                gated,
                jax.ShapeDtypeStruct(cell[8].shape, F32),
                jax.ShapeDtypeStruct(cell[9].shape, F32),
                jax.ShapeDtypeStruct(cell[10].shape, F32),
            ],
            [pltpu.VMEM((seqs, nv), F32)],
            state_cost,
            12 * MIB,
            received,
            *cell[8:],
        )

    if paired:
        pieces = [tokens] + peers([tokens] * (tp - 1), "tp", tp)
    else:
        stacked = lax.all_to_all(jnp.broadcast_to(tokens[None], (tp, rows, features)), "tp", 0, 0)
        pieces = [stacked.reshape(batch, features)]
    sums, x = call(
        functools.partial(first_body, len(pieces), 2 * heads),
        [payload, stream],
        project_scratch,
        project_cost,
        12 * MIB,
        *pieces,
        gains[0],
        *cells[0][1:5],
        small[0],
    )
    shared, *first = update(exchange_dp(sums), cells[0])
    sent, own = call(
        middle_body,
        [jax.ShapeDtypeStruct((batch, features), BF16), stream],
        [mix_scratch],
        mix_cost,
        8 * MIB,
        exchange_dp(shared),
        cells[0][7],
    )
    if paired:
        pieces = peers([sent] * (tp - 1), "tp", tp)
    else:
        own = jnp.zeros_like(own)
        pieces = [lax.all_to_all(jnp.broadcast_to(sent[None], (tp, batch, features)), "tp", 0, 0)]
    sums, x = call(
        functools.partial(second_body, len(pieces), 2 * heads),
        [payload, stream],
        project_scratch,
        project_cost,
        12 * MIB,
        x,
        own,
        *pieces,
        gains[1],
        *cells[1][1:5],
        small[1],
    )
    shared, *second = update(exchange_dp(sums), cells[1])
    block = jax.ShapeDtypeStruct((rows, features), BF16)
    if paired:
        outs = [jax.ShapeDtypeStruct((rows, features), F32)] + [block] * (tp - 1)
    else:
        outs = [jax.ShapeDtypeStruct((tp, rows, features), BF16)]
    sent = call(
        functools.partial(last_body, paired, tp),
        outs,
        [mix_scratch, pltpu.VMEM((batch, features), F32)],
        mix_cost,
        8 * MIB,
        exchange_dp(shared),
        cells[1][7],
    )
    if paired:
        pieces = [sent[0]] + peers(sent[1:], "tp", tp)
    else:
        pieces = [lax.all_to_all(sent[0], "tp", 0, 0)]
    (hidden,) = call(final_body, [block], [], rows * features, 2 * MIB, x, *pieces)
    return (hidden, *first, *second)


def solution(mesh):
    sizes = dict(mesh.shape)
    weight = P("dp", "tp")
    cell = (
        P("dp"),
        weight,
        weight,
        weight,
        weight,
        P("dp", None),
        P("dp", None),
        P("tp", "dp"),
        P("dp", "tp", None, None),
        P("dp", "tp", None),
        P("dp", "tp"),
    )
    states = cell[-3:]
    return jax.shard_map(
        lambda *args: per_device(sizes, *args),
        mesh=mesh,
        in_specs=(P("tp", "dp"), *cell, *cell),
        out_specs=(P("tp", "dp"), *states, *states),
        check_vma=False,
    )
```

```python
import functools

import jax
import jax.numpy as jnp
from jax import lax
from jax.experimental import pallas as pl
from jax.experimental.pallas import tpu as pltpu
from jax.sharding import PartitionSpec as P

eps = 1e-06
LANES = 128
F32 = jnp.float32
BF16 = jnp.bfloat16
NT = (((1,), (1,)), ((), ()))
TN = (((0,), (0,)), ((), ()))
MIB = 1 << 20
PREPARE_COST = 4 * 10**9


def pairwise(size):
    return size <= 4 and size & (size - 1) == 0


def peers(pieces, axis, size):
    order = sorted(range(1, size), key=lambda k: -bin(k).count("1"))
    got = {}
    for k in order:
        got[k] = lax.ppermute(pieces[k - 1], axis, [(i, i ^ k) for i in range(size)])
    return [got[k] for k in range(1, size)]


def split(x):
    high = x.astype(BF16)
    return high, (x - high.astype(F32)).astype(BF16)


def call(body, outs, scratch, cost, limit, *args):
    return pl.pallas_call(
        body,
        out_shape=outs,
        in_specs=[pl.BlockSpec(memory_space=pltpu.VMEM)] * len(args),
        out_specs=[pl.BlockSpec(memory_space=pltpu.VMEM)] * len(outs),
        scratch_shapes=scratch,
        cost_estimate=pl.CostEstimate(flops=cost, bytes_accessed=cost // 16, transcendentals=0),
        compiler_params=pltpu.CompilerParams(vmem_limit_bytes=limit),
    )(*args)


def pick(blocks, index):
    chosen = blocks[0]
    for j in range(1, len(blocks)):
        chosen = jnp.where(index == j, blocks[j], chosen)
    return chosen


def place(piece_refs, target):
    rows = piece_refs[0].shape[0]
    blocks = [piece[...].astype(F32) for piece in piece_refs]
    me = lax.axis_index("tp")
    for j in range(len(blocks)):
        target[j * rows : (j + 1) * rows, :] = pick(blocks, me ^ j)


def row_blocks(ref, rows):
    whole = ref[...].astype(F32)
    return [whole[j * rows : (j + 1) * rows, :] for j in range(ref.shape[0] // rows)]


def project(x, gain_ref, weights, small_ref, payload_ref, y_ref, narrow):
    batch = x.shape[0]
    squares = jnp.sum(x * x, axis=1, keepdims=True)
    scaled = (x * gain_ref[...]).astype(BF16)
    at = 0
    for w_ref in weights:
        width = w_ref.shape[1]
        y_ref[:, at : at + width] = jnp.dot(scaled, w_ref[...], preferred_element_type=F32)
        at += width
    gates = lax.dot_general(scaled, small_ref[...].astype(BF16), NT, preferred_element_type=F32)
    lane = lax.broadcasted_iota(jnp.int32, (batch, LANES), 1)
    gates = jnp.where(lane == narrow, squares, gates)
    high = gates.astype(BF16).astype(F32)
    y_ref[:, at : at + LANES] = high
    y_ref[:, at + LANES : at + 2 * LANES] = gates - high
    count, seqs, _ = payload_ref.shape
    for d in range(count):
        payload_ref[d] = y_ref[d * seqs : (d + 1) * seqs, :].astype(BF16)


def first_body(n_pieces, narrow, *refs):
    pieces = refs[:n_pieces]
    gain_ref, wq, wk, wv, wo, small_ref, payload_ref, stream_ref, y_ref = refs[n_pieces:]
    if n_pieces == 1:
        whole = pieces[0][...].astype(F32)
        stream_ref[...] = whole
    else:
        place(pieces, stream_ref)
    project(stream_ref[...], gain_ref, (wq, wk, wv, wo), small_ref, payload_ref, y_ref, narrow)


def second_body(n_pieces, narrow, *refs):
    stream_in, own_ref = refs[:2]
    pieces = refs[2 : 2 + n_pieces]
    gain_ref, wq, wk, wv, wo, small_ref, payload_ref, stream_ref, y_ref = refs[2 + n_pieces :]
    total = own_ref[...]
    for piece in pieces:
        if len(piece.shape) == 3:
            total = total + jnp.sum(piece[...].astype(F32), axis=0)
        else:
            total = total + piece[...].astype(F32)
    x = (stream_in[...] + total).astype(BF16).astype(F32)
    stream_ref[...] = x
    project(x, gain_ref, (wq, wk, wv, wo), small_ref, payload_ref, y_ref, narrow)


def read_body(
    width, received_ref, cell_ref, norm_ref, stab_ref,
    gated_ref, stab_out, gates_out, keys_out, values_out, read_ref,
):
    seqs, heads, dhv, dhk = cell_ref.shape
    nk, nv = heads * dhk, heads * dhv
    total = received_ref[0].astype(F32)
    for d in range(1, received_ref.shape[0]):
        total = total + received_ref[d].astype(F32)
    base = 2 * (nk + nv)
    small = total[:, base : base + LANES] + total[:, base + LANES : base + 2 * LANES]
    scale = lax.rsqrt(small[:, 2 * heads : 2 * heads + 1] / width + eps)
    small = small * scale
    input_pre = small[:, :heads]
    forget_pre = small[:, heads : 2 * heads]
    log_forget = jnp.minimum(forget_pre, 0.0) - jnp.log1p(jnp.exp(-jnp.abs(forget_pre)))
    kept = log_forget + stab_ref[...]
    stab_next = jnp.maximum(kept, input_pre)
    stab_out[...] = stab_next
    retain = jnp.exp(kept - stab_next)
    admitted = jnp.exp(input_pre - stab_next)
    gates_out[0] = retain
    gates_out[1] = admitted
    queries = total[:, :nk] * (scale * dhk ** (-0.5))
    keys = total[:, nk : 2 * nk] * scale
    values = total[:, 2 * nk : 2 * nk + nv] * scale
    keys_out[...] = keys
    values_out[...] = values
    gate = jax.nn.sigmoid(total[:, 2 * nk + nv : base] * scale)
    row = lax.broadcasted_iota(jnp.int32, (8, dhk), 0)
    for s in range(seqs):
        for h in range(heads):
            keep = retain[s : s + 1, h : h + 1]
            admit = admitted[s : s + 1, h : h + 1]
            query = queries[s : s + 1, h * dhk : (h + 1) * dhk]
            key = keys[s : s + 1, h * dhk : (h + 1) * dhk]
            value = values[s : s + 1, h * dhv : (h + 1) * dhv]
            matched = jnp.sum(key * query, axis=1, keepdims=True)
            stored = jnp.sum(norm_ref[s, h : h + 1, :] * query, axis=1, keepdims=True)
            bound = jnp.maximum(jnp.abs(keep * stored + admit * matched), 1.0)
            query_high = query.astype(BF16).astype(F32)
            asks = jnp.where(row == 0, query_high, jnp.where(row == 1, query - query_high, 0.0))
            asks = asks.astype(BF16)
            cell = cell_ref[s, h]
            cell_high = cell.astype(BF16)
            read = lax.dot_general(asks, cell_high, NT, preferred_element_type=F32)
            low = (cell - cell_high.astype(F32)).astype(BF16)
            read = read + lax.dot_general(asks, low, NT, preferred_element_type=F32)
            numerator = keep * jnp.sum(read, axis=0, keepdims=True) + (admit * matched) * value
            read_ref[s : s + 1, h * dhv : (h + 1) * dhv] = numerator / bound
    gated = (read_ref[...] * gate).astype(BF16)
    for d in range(gated_ref.shape[0]):
        gated_ref[d] = gated


def store_body(cell_ref, norm_ref, gates_ref, keys_ref, values_ref, cell_out, norm_out):
    seqs, heads, dhv, dhk = cell_ref.shape
    retain, admitted = gates_ref[0], gates_ref[1]
    row = lax.broadcasted_iota(jnp.int32, (8, dhk), 0)
    row_v = lax.broadcasted_iota(jnp.int32, (8, dhv), 0)
    for s in range(seqs):
        for h in range(heads):
            keep = retain[s : s + 1, h : h + 1]
            admit = admitted[s : s + 1, h : h + 1]
            key = keys_ref[s : s + 1, h * dhk : (h + 1) * dhk]
            value = values_ref[s : s + 1, h * dhv : (h + 1) * dhv] * admit
            norm_out[s, h : h + 1, :] = keep * norm_ref[s, h : h + 1, :] + admit * key
            key_high = key.astype(BF16).astype(F32)
            value_high = value.astype(BF16).astype(F32)
            left = jnp.where(row_v < 2, value_high, jnp.where(row_v < 4, value - value_high, 0.0))
            right = jnp.where(row & 1 == 0, key_high, key - key_high)
            outer = lax.dot_general(
                left.astype(BF16), right.astype(BF16), TN, preferred_element_type=F32
            )
            cell_out[s, h] = keep * cell_ref[s, h] + outer


def mix(gathered_ref, w_ref, x_ref):
    count, seqs, _ = gathered_ref.shape
    for d in range(count):
        x_ref[d * seqs : (d + 1) * seqs, :] = gathered_ref[d].astype(F32)
    return jnp.dot(x_ref[...].astype(BF16), w_ref[...], preferred_element_type=F32)


def middle_body(gathered_ref, w_ref, sent_ref, own_ref, x_ref):
    partial = mix(gathered_ref, w_ref, x_ref)
    own_ref[...] = partial
    sent_ref[...] = partial.astype(BF16)


def last_body(paired, size, gathered_ref, w_ref, *refs):
    x_ref, y_ref = refs[-2:]
    y_ref[...] = mix(gathered_ref, w_ref, x_ref)
    if not paired:
        sent_ref = refs[0]
        rows = sent_ref.shape[1]
        for k in range(size):
            sent_ref[k] = y_ref[k * rows : (k + 1) * rows, :].astype(BF16)
        return
    rows = refs[0].shape[0]
    blocks = row_blocks(y_ref, rows)
    me = lax.axis_index("tp")
    for k in range(size):
        refs[k][...] = pick(blocks, me ^ k).astype(refs[k].dtype)


def final_body(stream_ref, *refs):
    hidden_ref = refs[-1]
    rows = hidden_ref.shape[0]
    total = pick(row_blocks(stream_ref, rows), lax.axis_index("tp"))
    for piece in refs[:-1]:
        if len(piece.shape) == 3:
            total = total + jnp.sum(piece[...].astype(F32), axis=0)
        else:
            total = total + piece[...].astype(F32)
    hidden_ref[...] = total.astype(BF16)


def open_body(ref):
    ref[...] = jnp.zeros_like(ref)


def prepare_body(heads, *refs):
    refs = refs[1:]
    count = len(refs) // 5
    ins, outs = refs[: 3 * count], refs[3 * count :]
    me = lax.axis_index("tp")
    for c in range(count):
        gain_ref, input_ref, forget_ref = ins[3 * c : 3 * c + 3]
        gain_out, small_ref = outs[2 * c : 2 * c + 2]
        gain_out[...] = gain_ref[...].astype(F32)[None, :]
        rows = [pick(row_blocks(w, heads), me) for w in (input_ref, forget_ref)]
        small_ref[...] = jnp.zeros_like(small_ref)
        for j, block in enumerate(rows):
            small_ref[j * heads : (j + 1) * heads, :] = block.astype(F32)


def per_device(sizes, tokens, *args):
    tp, dp = sizes["tp"], sizes["dp"]
    paired = pairwise(tp)
    rows, features = tokens.shape
    batch = rows * tp
    cells = (args[:11], args[11:])
    seqs, heads, dhv, dhk = cells[0][8].shape
    nk, nv = heads * dhk, heads * dhv
    payload_width = 2 * (nk + nv) + 2 * LANES
    payload = jax.ShapeDtypeStruct((dp, seqs, payload_width), BF16)
    stream = jax.ShapeDtypeStruct((batch, features), F32)
    gated = jax.ShapeDtypeStruct((dp, seqs, nv), BF16)
    opened = call(open_body, [jax.ShapeDtypeStruct((8, LANES), F32)], [], PREPARE_COST, MIB)
    prepared = call(
        functools.partial(prepare_body, heads),
        [
            jax.ShapeDtypeStruct((1, features), F32),
            jax.ShapeDtypeStruct((LANES, features), F32),
        ]
        * 2,
        [],
        PREPARE_COST,
        4 * MIB,
        *opened,
        *(x for cell in cells for x in (cell[0], cell[5].T, cell[6].T)),
    )
    gains, small = prepared[0::2], prepared[1::2]
    project_scratch = [pltpu.VMEM((batch, payload_width), F32)]
    project_cost = 2 * batch * features * payload_width
    mix_scratch = pltpu.VMEM((batch, nv), F32)
    mix_cost = 2 * batch * features * nv
    state_cost = 16 * seqs * nv * dhk

    def exchange_dp(x):
        return lax.all_to_all(x, "dp", 0, 0)

    def read(received, cell):
        gated_rows, stab, gates, keys, values = call(
            functools.partial(read_body, features * dp),
            [
                gated,
                jax.ShapeDtypeStruct(cell[10].shape, F32),
                jax.ShapeDtypeStruct((2, *cell[10].shape), F32),
                jax.ShapeDtypeStruct((seqs, nk), F32),
                jax.ShapeDtypeStruct((seqs, nv), F32),
            ],
            [pltpu.VMEM((seqs, nv), F32)],
            state_cost,
            8 * MIB,
            received,
            *cell[8:],
        )
        cell_next, norm_next = call(
            store_body,
            [
                jax.ShapeDtypeStruct(cell[8].shape, F32),
                jax.ShapeDtypeStruct(cell[9].shape, F32),
            ],
            [],
            state_cost,
            8 * MIB,
            *cell[8:10],
            gates,
            keys,
            values,
        )
        return gated_rows, cell_next, norm_next, stab

    if paired:
        pieces = [tokens] + peers([tokens] * (tp - 1), "tp", tp)
    else:
        stacked = lax.all_to_all(jnp.broadcast_to(tokens[None], (tp, rows, features)), "tp", 0, 0)
        pieces = [stacked.reshape(batch, features)]
    sums, x = call(
        functools.partial(first_body, len(pieces), 2 * heads),
        [payload, stream],
        project_scratch,
        project_cost,
        12 * MIB,
        *pieces,
        gains[0],
        *cells[0][1:5],
        small[0],
    )
    shared, *first = read(exchange_dp(sums), cells[0])
    sent, own = call(
        middle_body,
        [jax.ShapeDtypeStruct((batch, features), BF16), stream],
        [mix_scratch],
        mix_cost,
        8 * MIB,
        exchange_dp(shared),
        cells[0][7],
    )
    if paired:
        pieces = peers([sent] * (tp - 1), "tp", tp)
    else:
        own = jnp.zeros_like(own)
        pieces = [lax.all_to_all(jnp.broadcast_to(sent[None], (tp, batch, features)), "tp", 0, 0)]
    pieces, first = lax.optimization_barrier((pieces, first))
    sums, x = call(
        functools.partial(second_body, len(pieces), 2 * heads),
        [payload, stream],
        project_scratch,
        project_cost,
        12 * MIB,
        x,
        own,
        *pieces,
        gains[1],
        *cells[1][1:5],
        small[1],
    )
    shared, *second = read(exchange_dp(sums), cells[1])
    block = jax.ShapeDtypeStruct((rows, features), BF16)
    if paired:
        outs = [jax.ShapeDtypeStruct((rows, features), F32)] + [block] * (tp - 1)
    else:
        outs = [jax.ShapeDtypeStruct((tp, rows, features), BF16)]
    sent = call(
        functools.partial(last_body, paired, tp),
        outs,
        [mix_scratch, pltpu.VMEM((batch, features), F32)],
        mix_cost,
        8 * MIB,
        exchange_dp(shared),
        cells[1][7],
    )
    if paired:
        pieces = [sent[0]] + peers(sent[1:], "tp", tp)
    else:
        pieces = [lax.all_to_all(sent[0], "tp", 0, 0)]
    (hidden,) = call(final_body, [block], [], rows * features, 2 * MIB, x, *pieces)
    return (hidden, *first, *second)


def solution(mesh):
    sizes = dict(mesh.shape)
    weight = P("dp", "tp")
    cell = (
        P("dp"),
        weight,
        weight,
        weight,
        weight,
        P("dp", None),
        P("dp", None),
        P("tp", "dp"),
        P("dp", "tp", None, None),
        P("dp", "tp", None),
        P("dp", "tp"),
    )
    states = cell[-3:]
    return jax.shard_map(
        lambda *args: per_device(sizes, *args),
        mesh=mesh,
        in_specs=(P("tp", "dp"), *cell, *cell),
        out_specs=(P("tp", "dp"), *states, *states),
        check_vma=False,
    )
```
